1024 devices in a mesh: ep: 64 (over z, y), tp: 16 (over x, core).
Axes of the slice: x: 8, y: 8, z: 8, core: 2. Of those that a mesh axis runs over, the one named last changes fastest.
Arguments:
- tokens: bfloat16 [8192, 2048], P('ep', 'tp'), may hold values from -6 to 6
- norm_gain: bfloat16 [2048], P('tp'), may hold values from 0.099609375 to 1.8984375
- routes: int32 [8192, 2], P('ep'), may hold values from 0 to 63, as said below
- gate_weights: float32 [8192, 2], P('ep'), may hold values from 0.1 to 1
- w_gate: bfloat16 [64, 2048, 4096], P('ep', None, 'tp'), may hold values from -0.125 to 0.125
- w_up: bfloat16 [64, 2048, 4096], P('ep', None, 'tp'), may hold values from -0.125 to 0.125
- w_down: bfloat16 [64, 4096, 2048], P('ep', 'tp'), may hold values from -0.875 to 0.875
- out_gain: bfloat16 [2048], P('tp'), may hold values from 0.099609375 to 1.8984375
Outputs:
- mixed: bfloat16 [8192, 2048], P('ep', 'tp')
The draws below stay inside these ranges and needn't reach their ends.
Inputs may be any that keep to these rules, and one draw needn't show every extreme that they name: `routes`: each row names 2 different experts of one group (their quotients by 8 agree). In each aligned block of 128 rows no expert is named by more than 8 rows, and in every block some expert is named by exactly 8 rows.
All inputs are finite; a program needn't handle non-finite values.
Results may differ from the reference program's by a relative error of at most 0.019.
Values may be sent and summed in bfloat16 or wider, within the bound.
A program may use at most 32 MiB of HBM per device.

```python
import math
import jax
import jax.numpy as jnp
from jax import lax

D = 2048
FF = 4096
EPG = 8
TOPK = 2
TOK_DEV = 128
EXPERTS = 64
GROUPS = 8
MEAN = 4
CAP = 8
TOKENS = 8192
N_EP = 64
N_TP = 16


def draw_routes(key, part):
    folded = jax.random.fold_in(key, 5)
    k_pop, k_jit, k_perm = jax.random.split(folded, 3)
    popular = jax.random.randint(k_pop, (EXPERTS,), 0, 4)
    jitter = jax.random.randint(k_jit, (N_EP, EXPERTS), 0, 3)
    expert_ids = jnp.arange(EXPERTS, dtype=jnp.int32)
    scores = (popular[None, :] * 4 + jitter) * EXPERTS + expert_ids[None, :]
    sorted_ids = jnp.argsort(scores, axis=1)
    ranking = jnp.argsort(sorted_ids, axis=1)
    quarter = ranking * 4 // EXPERTS
    counts = jnp.where(quarter == 3, 2 * MEAN, jnp.where(quarter == 2, MEAN, MEAN // 2)).astype(jnp.int32)
    group_copies = counts.reshape(N_EP, GROUPS, EPG).sum(axis=2)
    group_tokens = group_copies // 2
    token_end = jnp.cumsum(group_tokens, axis=1)
    token_start = token_end - group_tokens
    copy_start = jnp.cumsum(group_copies, axis=1) - group_copies
    expert_end = jnp.cumsum(counts, axis=1)
    positions = jnp.arange(TOK_DEV, dtype=jnp.int32)
    group_of = jnp.sum(positions[None, :, None] >= token_end[:, None, :], axis=2).astype(jnp.int32)
    within = positions[None, :] - jnp.take_along_axis(token_start, group_of, axis=1)
    first_copy = jnp.take_along_axis(copy_start, group_of, axis=1) + within
    second_copy = first_copy + jnp.take_along_axis(group_tokens, group_of, axis=1)

    def owner_of(copies):
        return jnp.sum(copies[:, :, None] >= expert_end[:, None, :], axis=2).astype(jnp.int32)
    chosen = jnp.stack([owner_of(first_copy), owner_of(second_copy)], axis=2)
    shuffle = jax.random.randint(k_perm, (N_EP, TOK_DEV), 0, 1 << 20) * TOK_DEV + positions[None, :]
    shuffled_order = jnp.argsort(shuffle, axis=1)
    chosen = jnp.take_along_axis(chosen, shuffled_order[:, :, None], axis=1)
    return chosen.reshape(N_EP * TOK_DEV, 2).astype(jnp.int32)


def draw_w_down(key, part):
    k_base, k_rough = jax.random.split(jax.random.fold_in(key, 7))
    column = jnp.arange(D, dtype=jnp.float32) / D
    base = jnp.clip(jax.random.normal(k_base, (EXPERTS, FF, D), jnp.float32), -4.0, 4.0)
    rising = 10.0 ** column
    rough = jax.random.uniform(k_rough, (D,), jnp.float32, 0.6, 1.4)
    return (base * (rising * rough / FF ** 0.5)[None, None, :]).astype(jnp.bfloat16)


def block_levels(own_key, shape, pieces, least, largest):
    def one(axis_at, parts):
        draws = jax.random.uniform(jax.random.fold_in(jax.random.fold_in(own_key, 6), axis_at), (parts,), jnp.float32, least / len(pieces), largest / len(pieces))
        return jnp.repeat(jnp.exp(draws), shape[axis_at] // parts).reshape((-1,) + (1,) * (len(shape) - axis_at - 1))

    gain = one(*pieces[0])
    for cut in pieces[1:]:
        gain = gain * one(*cut)
    return gain


def bell_draw(rng, extent, width, limit, shards=(), held_as=jnp.bfloat16):
    factor_of = block_levels(rng, extent, shards, -0.22, 0.18) if shards else 1.0
    result = jax.random.normal(rng, extent, jnp.float32) * width * factor_of
    return jnp.minimum(jnp.maximum(result, -limit), limit).astype(held_as)


def setup_inputs(seed: int = 0) -> dict:
    keys = jax.random.split(jax.random.key(seed), 9)
    tokens = bell_draw(keys[0], (TOKENS, D), 1.0, 6.0, ((0, 64), (1, 16)))
    norm_gain = jnp.clip(1.0 + 0.18 * jax.random.normal(keys[1], (D,), jnp.float32), 0.099609375, 1.8984375).astype(jnp.bfloat16)
    routes = draw_routes(jax.random.fold_in(keys[8], 71), 0)
    gate_weights = jnp.clip(jnp.exp(math.log(1.0) - 2.3025851 * jax.random.uniform(keys[3], (TOKENS, TOPK), jnp.float32) ** block_levels(keys[3], (TOKENS, TOPK), ((0, 64),), -0.2, 0.2)), 0.1, 1.0)
    w_gate = bell_draw(keys[4], (EXPERTS, D, FF), D ** -0.5, 0.125, ((0, 64), (2, 16)))
    w_up = bell_draw(keys[5], (EXPERTS, D, FF), D ** -0.5, 0.125, ((0, 64), (2, 16)))
    w_down = draw_w_down(jax.random.fold_in(keys[8], 71), 0)
    out_gain = jnp.clip(1.0 + 0.18 * jax.random.normal(keys[7], (D,), jnp.float32), 0.099609375, 1.8984375).astype(jnp.bfloat16)
    return dict(tokens=tokens, norm_gain=norm_gain, routes=routes, gate_weights=gate_weights, w_gate=w_gate, w_up=w_up, w_down=w_down, out_gain=out_gain)


epsilon = 1e-06

def route_slots(routes):
    blocks = routes.reshape(N_EP, TOK_DEV * TOPK)
    onehot = (blocks[:, :, None] == jnp.arange(EXPERTS, dtype=jnp.int32)[None, None, :]).astype(jnp.int32)
    before = jnp.cumsum(onehot, axis=1) - onehot
    return lax.optimization_barrier(jnp.sum(before * onehot, axis=2)).astype(jnp.int32)

def reference(tokens, norm_gain, routes, gate_weights, w_gate, w_up, w_down, out_gain):
    x_float = tokens.astype(jnp.float32)
    scale_in = lax.rsqrt(lax.optimization_barrier(jnp.mean(x_float * x_float, axis=1, keepdims=True)) + epsilon)
    normed = (x_float * scale_in * norm_gain.astype(jnp.float32)).astype(jnp.bfloat16)
    slot_index = route_slots(routes)
    expert_ids = routes.reshape(N_EP, TOK_DEV * TOPK).astype(jnp.int32)
    source = jnp.arange(N_EP, dtype=jnp.int32)[:, None]
    copy_ids = jnp.arange(TOK_DEV * TOPK, dtype=jnp.int32)[None, :]
    token_ids = (source * TOK_DEV + copy_ids // TOPK).astype(jnp.int32)
    buffer_pos = (source * CAP + slot_index).astype(jnp.int32)
    table = jnp.full((EXPERTS, N_EP * CAP), TOKENS, jnp.int32).at[expert_ids, buffer_pos].set(token_ids)
    padded = jnp.concatenate([normed, jnp.zeros((1, D), jnp.bfloat16)], axis=0)

    def expert(inputs):
        row_table, gate_mat, up_mat, down_mat = inputs
        arrived = padded[row_table]
        gate_sum = jnp.dot(arrived, gate_mat, preferred_element_type=jnp.float32)
        up_sum = jnp.dot(arrived, up_mat, preferred_element_type=jnp.float32)
        hidden = (jax.nn.silu(gate_sum) * up_sum).astype(jnp.bfloat16)
        hidden_blocks = hidden.reshape(N_EP * CAP, N_TP, FF // N_TP).astype(jnp.float32)
        down_blocks = down_mat.reshape(N_TP, FF // N_TP, D).astype(jnp.float32)
        partial_value = jnp.einsum('rtf,tfd->trd', hidden_blocks, down_blocks).astype(jnp.bfloat16)
        partial_value = lax.optimization_barrier(partial_value)
        return lax.optimization_barrier(jnp.sum(partial_value.astype(jnp.float32), axis=0)).astype(jnp.bfloat16)
    outputs = lax.map(expert, (table, w_gate, w_up, w_down))
    picked = outputs[expert_ids, buffer_pos].astype(jnp.float32).reshape(TOKENS, TOPK, D)
    combined = lax.optimization_barrier(jnp.sum(picked * gate_weights[:, :, None], axis=1))
    scale_out = lax.rsqrt(lax.optimization_barrier(jnp.mean(combined * combined, axis=1, keepdims=True)) + epsilon)
    return (combined * scale_out * out_gain.astype(jnp.float32)).astype(jnp.bfloat16)
```

```python
import functools

import jax
import jax.numpy as jnp
from jax import lax
from jax.experimental import pallas as pl
from jax.experimental.pallas import tpu as pltpu
from jax.sharding import PartitionSpec as P

MESH = pl.DeviceIdType.MESH
F32 = jnp.float32
BF16 = jnp.bfloat16
epsilon = 1e-06

NZ, NY, NX = 8, 8, 8
EP, TP = NZ * NY, 2 * NX
CAP = 8
ROWS = EP * CAP
NC = 4
SC = EP // NC
RC = SC * CAP
FAR = NX // 2
HOP_ORDER = (4, 3, 5, 2, 6, 1, 7, 0)


def rank_offset(r):
    return ((r % 2) * ((r + 1) // 2) + (1 - r % 2) * (8 - r // 2)) % 8


def chunk(k):
    return pl.ds(k * SC, SC)


def kernel(
    tok_ref, gain_ref, routes_ref, gw_ref, wg_hbm, wu_hbm, wd_hbm, og_ref,
    out_ref,
    send_s, xg, gains, xs, ss, wg, wu, wd, own, ps, pr, sb_r, sb_l, rb_r, rb_l, eo, cb, g_hi, g_lo, hid, nb,
    w_sem, a_send, a_recv, gain_send, gain_recv,
    r_send, l_send, p_send, x_recv, p_recv,
    ps_send, pr_recv, rr_send, rl_send, rr_recv, rl_recv,
    b_send, b_recv, n_send, n_recv,
):
    ep = lax.axis_index("ep")
    tp = lax.axis_index("tp")
    z, y = ep // NY, ep % NY
    x, c = tp // 2, tp % 2
    right = (ep, ((x + 1) % NX) * 2 + c)
    left = (ep, ((x + NX - 1) % NX) * 2 + c)
    partner = (ep, x * 2 + 1 - c)

    def expert_of(o):
        return ((z + rank_offset(o // NY)) % NZ) * NY + (y + rank_offset(o % NY)) % NY

    def source_of(o):
        return ((z + NZ - rank_offset(o // NY)) % NZ) * NY + (y + NY - rank_offset(o % NY)) % NY

    barrier = pltpu.get_barrier_semaphore()

    def greet_ep(o, carry):
        pl.semaphore_signal(barrier, inc=1, device_id=(expert_of(o), tp), device_id_type=MESH)
        return carry

    def greet_tp(q, carry):
        pl.semaphore_signal(barrier, inc=1, device_id=(ep, (tp + q) % TP), device_id_type=MESH)
        return carry

    lax.fori_loop(1, EP, greet_ep, 0)
    lax.fori_loop(1, TP, greet_tp, 0)

    for d in range(NX):
        chip = (x + d) % NX
        for p in range(2):
            block = chip * 2 + (c if p == 0 else 1 - c)
            at = pl.multiple_of(block * 128, 128)
            to = pl.ds((2 * d + p) * 128, 128)
            pltpu.make_async_copy(wg_hbm.at[pl.ds(at, 128)], wg.at[to], w_sem.at[0]).start()
            pltpu.make_async_copy(wu_hbm.at[pl.ds(at, 128)], wu.at[to], w_sem.at[1]).start()
            pltpu.make_async_copy(wd_hbm.at[:, pl.ds(at, 128)], wd.at[:, to], w_sem.at[2]).start()

    row = lax.broadcasted_iota(jnp.int32, (ROWS, 128), 0)
    o = row >> 3
    a, b = o >> 3, o & 7

    def vec_offset(r):
        return jnp.where((r & 1) == 1, (r + 1) >> 1, (8 - (r >> 1)) & 7)

    expert = (((z + vec_offset(a)) & 7) << 3) + ((y + vec_offset(b)) & 7)
    is0 = expert == routes_ref[0:1, :]
    is1 = expert == routes_ref[1:2, :]
    named = jnp.where(is0 | is1, 1.0, 0.0)
    upper = jnp.where(
        lax.broadcasted_iota(jnp.int32, (128, 128), 0) < lax.broadcasted_iota(jnp.int32, (128, 128), 1), 1.0, 0.0
    ).astype(BF16)
    before = jnp.dot(named.astype(BF16), upper, preferred_element_type=F32)
    here = (before == (row & 7).astype(F32)) & (named > 0.5)
    scatter = jnp.where(here, 1.0, 0.0).astype(BF16)
    outgoing = jnp.dot(scatter, tok_ref[...], preferred_element_type=F32)
    send_s[...] = outgoing.reshape(EP, CAP, 128).astype(BF16)
    xg[0, 0, 0] = outgoing[0:CAP].astype(BF16)
    gates = jnp.where(here, jnp.where(is0, gw_ref[0:1, :], gw_ref[1:2, :]), 0.0)
    hi = gates.astype(BF16)
    g_hi[...] = hi
    g_lo[...] = (gates - hi.astype(F32)).astype(BF16)
    gains[0] = jnp.broadcast_to(gain_ref[...].astype(F32), (CAP, 128)).astype(BF16)

    pl.semaphore_wait(barrier, EP + TP - 2)

    def send_gain(q, carry):
        pltpu.make_async_remote_copy(
            src_ref=gains.at[0], dst_ref=gains.at[q], send_sem=gain_send, recv_sem=gain_recv,
            device_id=(ep, (tp + TP - q) % TP), device_id_type=MESH,
        ).start()
        return carry

    def send_row(k):
        def body(i, carry):
            pltpu.make_async_remote_copy(
                src_ref=send_s.at[i], dst_ref=xg.at[0, 0, i], send_sem=a_send, recv_sem=a_recv.at[k],
                device_id=(expert_of(i), tp), device_id_type=MESH,
            ).start()
            return carry
        return body

    for k in range(NC):
        lax.fori_loop(max(1, k * SC), (k + 1) * SC, send_row(k), 0)
    lax.fori_loop(1, TP, send_gain, 0)

    def r_copy(h, k):
        return pltpu.make_async_remote_copy(
            src_ref=xg.at[(NX - h) % NX, 0, chunk(k)], dst_ref=xg.at[NX - h - 1, 0, chunk(k)],
            send_sem=r_send.at[h, k], recv_sem=x_recv.at[NX - h - 1, k], device_id=right, device_id_type=MESH,
        )

    def l_copy(h, k):
        return pltpu.make_async_remote_copy(
            src_ref=xg.at[h, 0, chunk(k)], dst_ref=xg.at[h + 1, 0, chunk(k)],
            send_sem=l_send.at[h, k], recv_sem=x_recv.at[h + 1, k], device_id=left, device_id_type=MESH,
        )

    def p_copy(d, k):
        return pltpu.make_async_remote_copy(
            src_ref=xg.at[d, 0, chunk(k)], dst_ref=xg.at[d, 1, chunk(k)],
            send_sem=p_send.at[d, k], recv_sem=p_recv.at[d, k], device_id=partner, device_id_type=MESH,
        )

    def goes_right(h, k):
        return h < FAR - 1 or (h == FAR - 1 and k % 2 == 0)

    def goes_left(h, k):
        return h < FAR - 1 or (h == FAR - 1 and k % 2 == 1)

    def take_in(d, p, k):
        value = xg[d, p, chunk(k)].astype(F32).reshape(RC, 128)
        square = value * value
        rows = pl.ds(k * RC, RC)
        if d == 0 and p == 0:
            ss[rows] = square
        else:
            ss[rows] += square
        q = gains_slot(d, p)
        gain = gains[q].astype(F32)[0:1]
        xs[rows, pl.ds((2 * d + p) * 128, 128)] = (value * gain).astype(BF16)

    def take_both(d, k):
        take_in(d, 0, k)
        p_copy(d, k).wait_recv()
        take_in(d, 1, k)

    def gains_slot(d, p):
        return 2 * d if p == 0 else (2 * d + 1 + TP - 2 * c) % TP

    steps = sorted(
        ((h * 3.5 + k * 1.5, h, k) for h in range(FAR + 1) for k in range(NC))
    )
    pending, taken = [], []
    for _, h, k in steps:
        pending, taken = taken, []
        if h == 0:
            first = max(1, k * SC)
            got = xg.at[0, 0, pl.ds(first, (k + 1) * SC - first)]
            pltpu.make_async_copy(got, got, a_recv.at[k]).wait()
            r_copy(0, k).start()
            l_copy(0, k).start()
            p_copy(0, k).start()
            taken.append((0, k))
        elif h < FAR:
            r_copy(h - 1, k).wait_recv()
            if goes_right(h, k):
                r_copy(h, k).start()
            p_copy(NX - h, k).start()
            l_copy(h - 1, k).wait_recv()
            if goes_left(h, k):
                l_copy(h, k).start()
            p_copy(h, k).start()
            taken.append((NX - h, k))
            taken.append((h, k))
        else:
            (r_copy if goes_right(h - 1, k) else l_copy)(h - 1, k).wait_recv()
            p_copy(FAR, k).start()
            taken.append((FAR, k))
        if (h, k) == (0, 0):
            rest = gains.at[pl.ds(1, TP - 1)]
            pltpu.make_async_copy(rest, rest, gain_recv).wait()
        for item in pending:
            take_both(*item)
    for item in taken:
        take_both(*item)

    pltpu.make_async_copy(wg_hbm, wg, w_sem.at[0]).wait()
    pltpu.make_async_copy(wu_hbm, wu, w_sem.at[1]).wait()
    pltpu.make_async_copy(wd_hbm, wd, w_sem.at[2]).wait()
    scale = lax.rsqrt(jnp.sum(ss[...], axis=1, keepdims=True) * (1.0 / (128 * TP)) + epsilon)
    gate = jnp.dot(xs[...], wg[...], preferred_element_type=F32) * scale
    up = jnp.dot(xs[...], wu[...], preferred_element_type=F32) * scale
    hid[...] = (gate / (1.0 + jnp.exp(-gate)) * up).astype(BF16)

    def ps_copy(d):
        return pltpu.make_async_remote_copy(
            src_ref=ps.at[d], dst_ref=pr.at[d], send_sem=ps_send.at[d], recv_sem=pr_recv.at[d],
            device_id=partner, device_id_type=MESH,
        )

    for d in HOP_ORDER:
        part = jnp.dot(hid[...], wd[:, pl.ds(d * 256, 256)], preferred_element_type=F32)
        ps[d] = part[:, 128:256].reshape(EP, CAP, 128).astype(BF16)
        ps_copy(d).start()
        own[d] = part[:, 0:128]

    def rr_copy(j, k):
        return pltpu.make_async_remote_copy(
            src_ref=sb_r.at[j, chunk(k)], dst_ref=rb_r.at[j, chunk(k)],
            send_sem=rr_send.at[j, k], recv_sem=rr_recv.at[j, k], device_id=right, device_id_type=MESH,
        )

    def rl_copy(j, k):
        return pltpu.make_async_remote_copy(
            src_ref=sb_l.at[j, chunk(k)], dst_ref=rb_l.at[j, chunk(k)],
            send_sem=rl_send.at[j, k], recv_sem=rl_recv.at[j, k], device_id=left, device_id_type=MESH,
        )

    def chip_part(d, k):
        return own[d, pl.ds(k * RC, RC)] + pr[d, chunk(k)].astype(F32).reshape(RC, 128)

    def has(j, k, side):
        return j > 0 or k % 2 == side

    def b_copy(i):
        return pltpu.make_async_remote_copy(
            src_ref=eo.at[i], dst_ref=cb.at[i], send_sem=b_send, recv_sem=b_recv,
            device_id=(source_of(i), tp), device_id_type=MESH,
        )

    def send_back(i, carry):
        b_copy(i).start()
        return carry

    for d in HOP_ORDER:
        ps_copy(d).wait_recv()

    order = tuple(reversed(range(NC)))
    steps = sorted((j * 3.5 + n * 1.0, j, k) for j in range(FAR + 1) for n, k in enumerate(order))
    for _, j, k in steps:
        if j < FAR:
            for side, copy, sb, rb, d in (
                (0, rr_copy, sb_r, rb_r, FAR - j),
                (1, rl_copy, sb_l, rb_l, (FAR + j) % NX),
            ):
                if not has(j, k, side):
                    continue
                total = chip_part(d, k)
                if j > 0 and has(j - 1, k, side):
                    copy(j - 1, k).wait_recv()
                    total = total + rb[j - 1, chunk(k)].astype(F32).reshape(RC, 128)
                sb[j, chunk(k)] = total.reshape(SC, CAP, 128).astype(BF16)
                copy(j, k).start()
        else:
            rr_copy(FAR - 1, k).wait_recv()
            rl_copy(FAR - 1, k).wait_recv()
            total = (
                chip_part(0, k)
                + rb_r[FAR - 1, chunk(k)].astype(F32).reshape(RC, 128)
                + rb_l[FAR - 1, chunk(k)].astype(F32).reshape(RC, 128)
            )
            result = total.reshape(SC, CAP, 128).astype(BF16)
            eo[chunk(k)] = result
            if k == 0:
                cb[0] = result[0]
            lax.fori_loop(max(1, k * SC), (k + 1) * SC, send_back, 0)

    rest = cb.at[pl.ds(1, EP - 1)]
    pltpu.make_async_copy(rest, rest, b_recv).wait()
    back = cb[...].astype(F32).reshape(ROWS, 128).astype(BF16)
    across = (((0,), (0,)), ((), ()))
    combined = lax.dot_general(g_hi[...], back, across, preferred_element_type=F32) + lax.dot_general(
        g_lo[...], back, across, preferred_element_type=F32
    )

    eye = lax.broadcasted_iota(jnp.int32, (128, 128), 0) == lax.broadcasted_iota(jnp.int32, (128, 128), 1)
    column = jnp.sum(combined * combined, axis=1, keepdims=True)
    line = jnp.sum(jnp.where(eye, column, 0.0), axis=0, keepdims=True)
    nb[0] = jnp.broadcast_to(line, (8, 128))

    def n_copy(q):
        return pltpu.make_async_remote_copy(
            src_ref=nb.at[0], dst_ref=nb.at[q], send_sem=n_send, recv_sem=n_recv,
            device_id=(ep, (tp + q) % TP), device_id_type=MESH,
        )

    def send_norm(q, carry):
        n_copy(q).start()
        return carry

    lax.fori_loop(1, TP, send_norm, 0)
    rest = nb.at[pl.ds(1, TP - 1)]
    pltpu.make_async_copy(rest, rest, n_recv).wait()
    total = jnp.sum(nb[...], axis=0)[0:1]
    scale_line = lax.rsqrt(total * (1.0 / (128 * TP)) + epsilon)
    scale_out = jnp.sum(jnp.where(eye, scale_line, 0.0), axis=1, keepdims=True)
    out_ref[...] = (combined * scale_out * og_ref[...].astype(F32)).astype(BF16)

    pltpu.make_async_copy(rest, rest, n_send).wait()
    sent = send_s.at[pl.ds(1, EP - 1)]
    pltpu.make_async_copy(sent, sent, a_send).wait()
    sent = eo.at[pl.ds(1, EP - 1)]
    pltpu.make_async_copy(sent, sent, b_send).wait()
    sent = gains.at[pl.ds(1, TP - 1)]
    pltpu.make_async_copy(sent, sent, gain_send).wait()
    for k in range(NC):
        for h in range(FAR):
            if goes_right(h, k):
                r_copy(h, k).wait_send()
            if goes_left(h, k):
                l_copy(h, k).wait_send()
        for d in range(NX):
            p_copy(d, k).wait_send()
        for j in range(FAR):
            if has(j, k, 0):
                rr_copy(j, k).wait_send()
            if has(j, k, 1):
                rl_copy(j, k).wait_send()
    for d in range(NX):
        ps_copy(d).wait_send()


def shards(tokens, norm_gain, routes, gate_weights, w_gate, w_up, w_down, out_gain):
    vmem = pl.BlockSpec(memory_space=pltpu.VMEM)
    hbm = pl.BlockSpec(memory_space=pl.ANY)
    dma = pltpu.SemaphoreType.DMA
    width = tokens.shape[1]
    features = width * TP
    units = w_gate.shape[2]
    return pl.pallas_call(
        kernel,
        out_shape=jax.ShapeDtypeStruct(tokens.shape, BF16),
        in_specs=[vmem, vmem, vmem, vmem, hbm, hbm, hbm, vmem],
        out_specs=vmem,
        scratch_shapes=[
            pltpu.VMEM((EP, CAP, width), BF16),
            pltpu.VMEM((NX, 2, EP, CAP, width), BF16),
            pltpu.VMEM((TP, CAP, width), BF16),
            pltpu.VMEM((ROWS, features), BF16),
            pltpu.VMEM((ROWS, width), F32),
            pltpu.VMEM((features, units), BF16),
            pltpu.VMEM((features, units), BF16),
            pltpu.VMEM((units, features), BF16),
            pltpu.VMEM((NX, ROWS, width), F32),
            pltpu.VMEM((NX, EP, CAP, width), BF16),
            pltpu.VMEM((NX, EP, CAP, width), BF16),
            pltpu.VMEM((FAR, EP, CAP, width), BF16),
            pltpu.VMEM((FAR, EP, CAP, width), BF16),
            pltpu.VMEM((FAR, EP, CAP, width), BF16),
            pltpu.VMEM((FAR, EP, CAP, width), BF16),
            pltpu.VMEM((EP, CAP, width), BF16),
            pltpu.VMEM((EP, CAP, width), BF16),
            pltpu.VMEM((ROWS, 128), BF16),
            pltpu.VMEM((ROWS, 128), BF16),
            pltpu.VMEM((ROWS, units), BF16),
            pltpu.VMEM((TP, 8, 128), F32),
            dma((3,)), dma, dma((NC,)), dma, dma,
            dma((FAR, NC)), dma((FAR, NC)), dma((NX, NC)), dma((NX, NC)), dma((NX, NC)),
            dma((NX,)), dma((NX,)), dma((FAR, NC)), dma((FAR, NC)), dma((FAR, NC)), dma((FAR, NC)),
            dma, dma, dma, dma,
        ],
        compiler_params=pltpu.CompilerParams(
            collective_id=0, has_side_effects=True, vmem_limit_bytes=60 * 1024 * 1024
        ),
        name="layer",
    )(
        tokens, norm_gain.reshape(1, -1), routes.T, gate_weights.T, w_gate[0], w_up[0], w_down[0],
        out_gain.reshape(1, -1),
    )


def solution(mesh):
    placed = (
        P("ep", "tp"),
        P("tp"),
        P("ep", None),
        P("ep", None),
        P("ep", None, "tp"),
        P("ep", None, "tp"),
        P("ep", "tp", None),
        P("tp"),
    )
    return jax.shard_map(
        shards, mesh=mesh, in_specs=placed, out_specs=P("ep", "tp"), check_vma=False
    )
```
